32 devices in a mesh: sp: 4 (over y, x), dp: 8 (over z, core).
Axes of the slice: x: 2, y: 2, z: 4, core: 2. Of those that a mesh axis runs over, the one named last changes fastest.
Arguments:
- tokens: bfloat16 [8, 1024, 2048], P('dp', 'sp'), may hold values from -200 to 200
- w_qdown: bfloat16 [2048, 512], P('dp'), may hold values from -0.125 to 0.125
- w_kvdown: bfloat16 [2048, 512], P('dp'), may hold values from -0.125 to 0.125
- w_rotary: bfloat16 [2048, 64], replicated, may hold values from -0.125 to 0.125
- q_gain: float32 [512], replicated, may hold values from 0.1 to 1.9
- kv_gain: float32 [512], replicated, may hold values from 0.1 to 1.9
- w_qup: bfloat16 [512, 3072], P('dp'), may hold values from -1 to 1
- w_kvup: bfloat16 [512, 4096], P('dp'), may hold values from -1 to 1
- w_out: bfloat16 [2048, 2048], P(None, 'dp'), may hold values from -0.125 to 0.125
- out_gain: float32 [2048], replicated, may hold values from 0.1 to 1.9
Outputs:
- mixed: bfloat16 [8, 1024, 2048], P('dp', 'sp')
The draws below stay inside these ranges and needn't reach their ends.
All inputs are finite; a program needn't handle non-finite values.
Results may differ from the reference program's by a relative error of at most 0.01.
The reference program's roundings to bfloat16 on the way count: a program that leaves them out, or rounds other values in their place, can miss the bound.
Values may be sent and summed in bfloat16 or wider, within the bound.
A program may use at most 128 MiB of HBM per device.

```python
import math
import jax
import jax.numpy as jnp
from jax import lax

D = 2048
HEADS = 16
Q_RANK = 512
KV_RANK = 512
NOPE = 128
ROPE = 64
VDIM = 128
LENGTH = 1024
BATCH = 8


def draw_tokens(key, part):
    value_key = jax.random.fold_in(key, 11)
    values = jnp.clip(jax.random.normal(value_key, (BATCH, LENGTH, D), jnp.float32), -6.0, 6.0)
    return values.astype(jnp.bfloat16)


def base_weight(key, salt, rank, width):
    normal = jax.random.normal(jax.random.fold_in(key, salt), (rank, HEADS, width), jnp.float32)
    return jnp.clip(normal, -4.0, 4.0) * rank ** (-0.5)


def draw_w_qup(key, part):
    values = base_weight(key, 41, Q_RANK, NOPE + ROPE)
    values = jnp.clip(values, -1.0, 1.0)
    return values.reshape(Q_RANK, HEADS * (NOPE + ROPE)).astype(jnp.bfloat16)


def draw_w_kvup(key, part):
    values = base_weight(key, 51, KV_RANK, NOPE + VDIM)
    values = jnp.clip(values, -1.0, 1.0)
    return values.reshape(KV_RANK, HEADS * (NOPE + VDIM)).astype(jnp.bfloat16)


def levels(rng, extent, split, least, largest):
    def one(axis_at, blocks):
        draws = jax.random.uniform(jax.random.fold_in(jax.random.fold_in(rng, 6), axis_at), (blocks,), jnp.float32, least / len(split), largest / len(split))
        return jnp.repeat(jnp.exp(draws), extent[axis_at] // blocks).reshape((-1,) + (1,) * (len(extent) - axis_at - 1))

    level = one(*split[0])
    for cut in split[1:]:
        level = level * one(*cut)
    return level


def centred(stream_key, extent, scale, reach, cuts=(), dtype=jnp.bfloat16):
    factor_of = levels(stream_key, extent, cuts, -0.22, 0.18) if cuts else 1.0
    result = jax.random.normal(stream_key, extent, jnp.float32) * scale * factor_of
    return jnp.minimum(jnp.maximum(result, -reach), reach).astype(dtype)


def setup_inputs(seed: int = 0) -> dict:
    arg_keys = jax.random.split(jax.random.key(seed), 11)
    return {
        "tokens": draw_tokens(jax.random.fold_in(arg_keys[10], 71), 0),
        "w_qdown": centred(arg_keys[1], (D, Q_RANK), D ** -0.5, 0.125, ((0, 8),)),
        "w_kvdown": centred(arg_keys[2], (D, KV_RANK), D ** -0.5, 0.125, ((0, 8),)),
        "w_rotary": centred(arg_keys[3], (D, ROPE), D ** -0.5, 0.125),
        "q_gain": jnp.clip(1.0 + 0.18 * jax.random.normal(arg_keys[4], (Q_RANK,), jnp.float32), 0.1, 1.9),
        "kv_gain": jnp.clip(1.0 + 0.18 * jax.random.normal(arg_keys[5], (KV_RANK,), jnp.float32), 0.1, 1.9),
        "w_qup": draw_w_qup(jax.random.fold_in(arg_keys[10], 71), 0),
        "w_kvup": draw_w_kvup(jax.random.fold_in(arg_keys[10], 71), 0),
        "w_out": centred(arg_keys[8], (HEADS * VDIM, D), (HEADS * VDIM) ** -0.5, 0.125, ((1, 8),)),
        "out_gain": jnp.clip(1.0 + 0.18 * jax.random.normal(arg_keys[9], (D,), jnp.float32), 0.1, 1.9),
    }


EPSILON = 1e-06
THETA = 10000.0

def norm_rows(values, gain):
    scale = lax.rsqrt(lax.optimization_barrier(jnp.mean(values * values, axis=-1, keepdims=True)) + EPSILON)
    return values * scale * gain

def rotate(values, cosine, sine):
    half = values.shape[-1] // 2
    first = values[..., :half]
    second = values[..., half:]
    return jnp.concatenate([first * cosine - second * sine, second * cosine + first * sine], axis=-1)

def reference(tokens, w_qdown, w_kvdown, w_rotary, q_gain, kv_gain, w_qup, w_kvup, w_out, out_gain):
    length = tokens.shape[1]
    positions = jnp.arange(length).astype(jnp.float32)
    freqs = THETA ** (-jnp.arange(0, ROPE, 2).astype(jnp.float32) / ROPE)
    angles = positions[:, None] * freqs[None, :]
    cosine = jnp.cos(angles)
    sine = jnp.sin(angles)
    block = math.gcd(length, 512)
    qk_width = NOPE + ROPE
    scaling = qk_width ** (-0.5)

    def one_sequence(sequence):
        q_lat = jnp.dot(sequence, w_qdown, preferred_element_type=jnp.float32)
        kv_lat = jnp.dot(sequence, w_kvdown, preferred_element_type=jnp.float32)
        q_norm = norm_rows(q_lat, q_gain).astype(jnp.bfloat16)
        kv_norm = norm_rows(kv_lat, kv_gain).astype(jnp.bfloat16)
        key_rot = rotate(jnp.dot(sequence, w_rotary, preferred_element_type=jnp.float32), cosine, sine).astype(jnp.bfloat16)
        q_full = jnp.dot(q_norm, w_qup, preferred_element_type=jnp.float32).reshape(length, HEADS, qk_width)
        q_turn = rotate(q_full[..., NOPE:], cosine[:, None, :], sine[:, None, :])
        queries = jnp.concatenate([q_full[..., :NOPE], q_turn], axis=-1).astype(jnp.bfloat16)
        keyval = jnp.dot(kv_norm, w_kvup, preferred_element_type=jnp.float32).astype(jnp.bfloat16)
        keyval = keyval.reshape(length, HEADS, NOPE + VDIM)
        keys_all = keyval[..., :NOPE].astype(jnp.float32)
        values_all = keyval[..., NOPE:].astype(jnp.float32)
        rot_all = key_rot.astype(jnp.float32)
        outputs = []
        for begin in range(0, length, block):
            finish = begin + block
            query_block = queries[begin:finish].astype(jnp.float32)
            scores = jnp.einsum('qhd,khd->hqk', query_block[..., :NOPE], keys_all[:finish])
            scores = scores + jnp.einsum('qhd,kd->hqk', query_block[..., NOPE:], rot_all[:finish])
            scores = scores * scaling
            query_pos = begin + jnp.arange(block)
            key_pos = jnp.arange(finish)
            allowed = key_pos[None, :] <= query_pos[:, None]
            scores = jnp.where(allowed[None], scores, -jnp.inf)
            top = lax.optimization_barrier(jnp.max(scores, axis=-1, keepdims=True))
            expo = jnp.exp(scores - top)
            weights = (expo / lax.optimization_barrier(jnp.sum(expo, axis=-1, keepdims=True))).astype(jnp.bfloat16)
            attended = jnp.einsum('hqk,khd->qhd', weights.astype(jnp.float32), values_all[:finish])
            outputs.append(attended.astype(jnp.bfloat16))
        attended_all = jnp.concatenate(outputs, axis=0).reshape(length, HEADS * VDIM)
        proj = jnp.dot(attended_all, w_out, preferred_element_type=jnp.float32)
        return norm_rows(proj, out_gain).astype(jnp.bfloat16)
    return lax.map(one_sequence, tokens)
```

```python
import functools
import math

import jax
import jax.numpy as jnp
import numpy as np
from jax import lax
from jax.experimental import pallas as pl
from jax.experimental.pallas import tpu as pltpu
from jax.sharding import PartitionSpec as P

HEADS = 16
NOPE = 128
ROPE = 64
VDIM = 128


EPSILON = 1e-06
THETA = 10000.0
LANES = 128
SUBLANES = 16
MESH = pl.DeviceIdType.MESH


def norm_rows(values, gain):
    scale = lax.rsqrt(jnp.mean(values * values, axis=-1, keepdims=True) + EPSILON)
    return values * scale * gain


def rotate(values, cosine, sine):
    half = values.shape[-1] // 2
    first = values[..., :half]
    second = values[..., half:]
    return jnp.concatenate(
        [first * cosine - second * sine, second * cosine + first * sine], axis=-1
    )


def turn_tables(offset, count):
    positions = (offset + jnp.arange(count)).astype(jnp.float32)
    freqs = THETA ** (-jnp.arange(0, ROPE, 2).astype(jnp.float32) / ROPE)
    angles = positions[:, None] * freqs[None, :]
    return (jnp.cos(angles), jnp.sin(angles))


def make_queries(q_full, cosine, sine, heads_here):
    rows = q_full.shape[0]
    shaped = q_full.reshape(rows, heads_here, NOPE + ROPE)
    turned = rotate(shaped[..., NOPE:], cosine[:, None, :], sine[:, None, :])
    joined = jnp.concatenate([shaped[..., :NOPE], turned], axis=-1)
    return joined.reshape(rows, heads_here * (NOPE + ROPE)).astype(jnp.bfloat16)


def attend(query_heads, keyval_heads, key_rot, heads_here):
    length = query_heads.shape[0]
    block = math.gcd(length, 512)
    scaling = (NOPE + ROPE) ** (-0.5)
    queries = query_heads.reshape(length, heads_here, NOPE + ROPE)
    keyval = keyval_heads.reshape(length, heads_here, NOPE + VDIM)
    keys_all = keyval[..., :NOPE]
    values_all = keyval[..., NOPE:]
    outputs = []
    for begin in range(0, length, block):
        finish = begin + block
        query_block = queries[begin:finish]
        scores = jnp.einsum(
            "qhd,khd->hqk",
            query_block[..., :NOPE],
            keys_all[:finish],
            preferred_element_type=jnp.float32,
        )
        scores = scores + jnp.einsum(
            "qhd,kd->hqk",
            query_block[..., NOPE:],
            key_rot[:finish],
            preferred_element_type=jnp.float32,
        )
        scores = scores * scaling
        query_pos = begin + jnp.arange(block)
        key_pos = jnp.arange(finish)
        allowed = key_pos[None, :] <= query_pos[:, None]
        scores = jnp.where(allowed[None], scores, -jnp.inf)
        top = jnp.max(scores, axis=-1, keepdims=True)
        expo = jnp.exp(scores - top)
        weights = (expo / jnp.sum(expo, axis=-1, keepdims=True)).astype(jnp.bfloat16)
        attended = jnp.einsum(
            "hqk,khd->qhd", weights, values_all[:finish], preferred_element_type=jnp.float32
        )
        outputs.append(attended.astype(jnp.bfloat16))
    return jnp.concatenate(outputs, axis=0).reshape(length, heads_here * VDIM)


def plain_body(tokens, w_qdown, w_kvdown, w_rotary, q_gain, kv_gain, w_qup, w_kvup, w_out, out_gain):
    own_rows = tokens[0]
    tok_count = own_rows.shape[0]
    sp_count = lax.axis_size("sp")
    sp_place = lax.axis_index("sp")
    length = tok_count * sp_count
    heads_here = HEADS // sp_count
    pieces = (
        lax.all_gather(w_qdown, "dp", axis=0, tiled=True),
        lax.all_gather(w_kvdown, "dp", axis=0, tiled=True),
    )
    q_lat = jnp.dot(own_rows, pieces[0], preferred_element_type=jnp.float32)
    kv_lat = jnp.dot(own_rows, pieces[1], preferred_element_type=jnp.float32)
    q_norm = norm_rows(q_lat, q_gain).astype(jnp.bfloat16)
    kv_norm = norm_rows(kv_lat, kv_gain).astype(jnp.bfloat16)
    own_cos, own_sin = turn_tables(sp_place * tok_count, tok_count)
    key_rot = rotate(
        jnp.dot(own_rows, w_rotary, preferred_element_type=jnp.float32), own_cos, own_sin
    ).astype(jnp.bfloat16)
    q_all, kv_all, rot_all = (
        lax.all_gather(q_norm, "sp", axis=0, tiled=True),
        lax.all_gather(kv_norm, "sp", axis=0, tiled=True),
        lax.all_gather(key_rot, "sp", axis=0, tiled=True),
    )
    q_width = heads_here * (NOPE + ROPE)
    kv_width = heads_here * (NOPE + VDIM)
    q_columns = lax.dynamic_slice_in_dim(w_qup, sp_place * q_width, q_width, 1)
    kv_columns = lax.dynamic_slice_in_dim(w_kvup, sp_place * kv_width, kv_width, 1)
    pieces = (
        lax.all_gather(q_columns, "dp", axis=0, tiled=True),
        lax.all_gather(kv_columns, "dp", axis=0, tiled=True),
    )
    q_full = jnp.dot(q_all, pieces[0], preferred_element_type=jnp.float32)
    kv_full = jnp.dot(kv_all, pieces[1], preferred_element_type=jnp.float32)
    all_cos, all_sin = turn_tables(0, length)
    query_heads = make_queries(q_full, all_cos, all_sin, heads_here)
    keyval_heads = kv_full.astype(jnp.bfloat16)
    attended = attend(query_heads, keyval_heads, rot_all, heads_here)
    merged = lax.all_to_all(attended, "sp", split_axis=0, concat_axis=1, tiled=True)
    proj = jnp.dot(
        merged, lax.all_gather(w_out, "dp", axis=1, tiled=True), preferred_element_type=jnp.float32
    )
    mixed = norm_rows(proj, out_gain).astype(jnp.bfloat16)
    return mixed[None]


def turn_table(length):
    positions = np.arange(length, dtype=np.float32)
    freqs = np.float32(THETA) ** (-np.arange(0, ROPE, 2).astype(np.float32) / np.float32(ROPE))
    angles = positions[:, None] * freqs[None, :].astype(np.float32)
    cosine, sine = np.cos(angles), np.sin(angles)
    return np.concatenate([cosine, cosine, sine, sine], axis=1).astype(np.float32)


class Copies:
    def __init__(self, send_sems, recv_sems):
        self.send_sems, self.recv_sems = send_sems, recv_sems
        self.used = 0
        self.sent = []

    def start(self, source, target, device):
        at = self.used
        self.used += 1
        copy = pltpu.make_async_remote_copy(
            src_ref=source,
            dst_ref=target,
            send_sem=self.send_sems.at[at],
            recv_sem=self.recv_sems.at[at],
            device_id=device,
            device_id_type=MESH,
        )
        copy.start()
        self.sent.append(copy)
        return copy


class PlaneSpread:
    def __init__(self, copies, place, view, rows):
        self.copies, self.place, self.view, self.rows = copies, place, view, rows

    def send(self):
        me, rows = self.place["me"], self.rows
        block = self.view(me, 0, rows)
        self.along_x = self.copies.start(block, block, {"sp": self.place["x"]})
        self.along_y = self.copies.start(block, block, {"sp": self.place["y"]})

    def relay(self):
        half = self.rows // 2
        self.along_x.wait_recv()
        block = self.view(self.place["x"], 0, half)
        self.first = self.copies.start(block, block, {"sp": self.place["y"]})
        self.along_y.wait_recv()
        block = self.view(self.place["y"], half, half)
        self.second = self.copies.start(block, block, {"sp": self.place["x"]})

    def finish(self):
        self.first.wait_recv()
        self.second.wait_recv()


class WeightGather:
    def __init__(self, copies, place, source, buffer):
        self.copies, self.place, self.source, self.buffer = copies, place, source, buffer
        self.rows = source.shape[0] // place["sp_count"]

    def piece(self, slot, owner, begin, count):
        start = pl.multiple_of(owner * self.rows + begin, SUBLANES)
        return self.buffer.at[slot, pl.ds(start, count), :]

    def start(self):
        place, rows = self.place, self.rows
        own = self.source.at[pl.ds(pl.multiple_of(place["me"] * rows, SUBLANES), rows), :]
        self.arrivals = []
        for step in range(1, place["z_count"]):
            target = self.piece(place["dp"], place["me"], 0, rows)
            device = {"dp": lax.rem(place["dp"] + 2 * step, place["dp_count"])}
            self.arrivals.append(self.copies.start(own, target, device))

    def keep(self):
        place = self.place
        self.crossed = [
            self.copies.start(self.source, self.buffer.at[place["dp"]], {"dp": place["core"]})
        ]
        self.buffer[place["dp"]] = self.source[...]

    def slot(self, step):
        place = self.place
        return lax.rem(place["dp"] + place["dp_count"] - 2 * step, place["dp_count"])

    def spread(self):
        self.planes = []
        for step in range(1, self.place["z_count"]):
            self.arrivals[step - 1].wait_recv()
            view = functools.partial(self.piece, self.slot(step))
            plane = PlaneSpread(self.copies, self.place, view, self.rows)
            plane.send()
            self.planes.append(plane)

    def relay(self):
        for plane in self.planes:
            plane.relay()

    def cross(self):
        for step in range(1, self.place["z_count"]):
            self.planes[step - 1].finish()
            block = self.buffer.at[self.slot(step)]
            self.crossed.append(self.copies.start(block, block, {"dp": self.place["core"]}))

    def finish(self):
        for copy in self.crossed:
            copy.wait_recv()


class ColumnGather:
    def __init__(self, copies, place, source, buffer):
        self.copies, self.place, self.source, self.buffer = copies, place, source, buffer
        width = buffer.shape[2]
        self.columns = pl.ds(pl.multiple_of(place["me"] * width, LANES), width)

    def start(self):
        place = self.place
        own = self.source.at[:, self.columns]
        target = self.buffer.at[place["dp"]]
        self.arrivals = []
        for step in range(1, place["z_count"]):
            device = {"dp": lax.rem(place["dp"] + 2 * step, place["dp_count"])}
            self.arrivals.append(self.copies.start(own, target, device))

    def keep(self):
        place = self.place
        own = self.source.at[:, self.columns]
        target = self.buffer.at[place["dp"]]
        self.crossed = [self.copies.start(own, target, {"dp": place["core"]})]
        self.buffer[place["dp"]] = self.source[:, self.columns]

    def cross(self):
        place = self.place
        for step in range(1, place["z_count"]):
            self.arrivals[step - 1].wait_recv()
            slot = lax.rem(place["dp"] + place["dp_count"] - 2 * step, place["dp_count"])
            block = self.buffer.at[slot]
            self.crossed.append(self.copies.start(block, block, {"dp": place["core"]}))

    def finish(self):
        for copy in self.crossed:
            copy.wait_recv()


def rotary_picks(rows, offset, skip):
    width = skip + 2 * ROPE
    row = lax.broadcasted_iota(jnp.int32, (rows, width), 0)
    col = lax.broadcasted_iota(jnp.int32, (rows, width), 1)
    half = ROPE // 2
    minus = (col >= skip + ROPE) & (col < skip + ROPE + half)
    origin = jnp.where(
        col < skip + ROPE, col, jnp.where(minus, col - half, col - ROPE - half)
    )
    sign = jnp.where(minus, -1.0, 1.0)
    return jnp.where(row == origin + offset, sign, 0.0).astype(jnp.bfloat16)


def turned(values, table):
    product = values * table
    return product + pltpu.roll(product, ROPE, axis=1)


def dot(left, right):
    return jnp.dot(left, right, preferred_element_type=jnp.float32)


def kernel(
    sp_count, dp_count,
    tokens, w_qdown, w_kvdown, w_rotary, q_gain, kv_gain, w_qup, w_kvup, w_out, out_gain, table,
    out,
    qd_all, kvd_all, qu_all, kvu_all, wo_all, q_lat, kv_lat,
    q_heads, k_heads, v_heads, qu_laid, attended, merged, proj,
    send_sems, recv_sems, back_send, back_recv,
):
    me = lax.axis_index("sp")
    dp = lax.axis_index("dp")
    place = {
        "me": me,
        "dp": dp,
        "sp_count": sp_count,
        "dp_count": dp_count,
        "z_count": dp_count // 2,
        "x": me + 1 - 2 * lax.rem(me, 2),
        "y": lax.rem(me + 2, sp_count),
        "core": dp + 1 - 2 * lax.rem(dp, 2),
    }
    count = tokens.shape[0]
    heads = q_heads.shape[0]
    rank = kvd_all.shape[2]

    barrier = pltpu.get_barrier_semaphore()
    peers = [{"sp": lax.rem(me + step, sp_count)} for step in range(1, sp_count)]
    peers += [{"dp": lax.rem(dp + 2 * step, dp_count)} for step in range(1, dp_count // 2)]
    peers += [{"dp": place["core"]}]
    for peer in peers:
        pl.semaphore_signal(barrier, inc=1, device_id=peer, device_id_type=MESH)
    pl.semaphore_wait(barrier, len(peers))

    copies = Copies(send_sems, recv_sems)
    kvd = WeightGather(copies, place, w_kvdown, kvd_all)
    qd = WeightGather(copies, place, w_qdown, qd_all)
    kvu = ColumnGather(copies, place, w_kvup, kvu_all)
    qu = ColumnGather(copies, place, w_qup, qu_all)
    wo = WeightGather(copies, place, w_out, wo_all)
    gathers = (kvd, qd, kvu, qu, wo)
    for gather in gathers:
        gather.start()
    for gather in gathers:
        gather.keep()

    own_table = table[pl.ds(pl.multiple_of(me * count, SUBLANES), count), :]
    rotary = dot(w_rotary[...], rotary_picks(ROPE, 0, 0)).astype(jnp.bfloat16)
    key_rot = turned(dot(tokens[...], rotary), own_table)
    lane = lax.broadcasted_iota(jnp.int32, key_rot.shape, 1)
    key_rot = jnp.where(lane < ROPE, key_rot, 0.0).astype(jnp.bfloat16)
    kv_lat[me, :, rank:] = key_rot

    kvd.spread()
    kvd.relay()
    qd.spread()
    kvd.cross()
    qd.relay()
    kvd.finish()
    down = kvd_all[...].reshape(-1, rank)
    kv_lat[me, :, :rank] = norm_rows(dot(tokens[...], down), kv_gain[...]).astype(jnp.bfloat16)

    def block_view(buffer, owner, begin, rows):
        return buffer.at[owner, pl.ds(begin, rows), :]

    kv_plane = PlaneSpread(copies, place, functools.partial(block_view, kv_lat), count)
    q_plane = PlaneSpread(copies, place, functools.partial(block_view, q_lat), count)
    kv_plane.send()
    qd.cross()
    qd.finish()
    down = qd_all[...].reshape(-1, qd_all.shape[2])
    q_lat[me] = norm_rows(dot(tokens[...], down), q_gain[...]).astype(jnp.bfloat16)
    q_plane.send()
    kv_plane.relay()

    qu.cross()
    kvu.cross()
    qu.finish()
    laid = qu_all[...].reshape(-1, qu_all.shape[2])
    head_width = NOPE + 2 * ROPE
    for head in range(heads):
        picks = rotary_picks(laid.shape[1], head * (NOPE + ROPE), NOPE)
        qu_laid[:, head * head_width : (head + 1) * head_width] = dot(laid, picks).astype(
            jnp.bfloat16
        )
    q_plane.relay()
    wo.spread()
    kvu.finish()
    kv_plane.finish()

    def make_keys(block, _):
        rows = pl.ds(pl.multiple_of(block * count, SUBLANES), count)
        latent = kv_lat[block]
        full = dot(latent[:, :rank], kvu_all[...].reshape(rank, -1)).astype(jnp.bfloat16)
        for head in range(heads):
            at = head * (NOPE + VDIM)
            k_heads[head, rows, :NOPE] = full[:, at : at + NOPE]
            k_heads[head, rows, NOPE:] = latent[:, rank:]
            v_heads[head, rows, :] = full[:, at + NOPE : at + NOPE + VDIM]
        return 0

    lax.fori_loop(0, sp_count, make_keys, 0)
    q_plane.finish()

    def make_block(block, _):
        rows = pl.ds(pl.multiple_of(block * count, SUBLANES), count)
        full = dot(q_lat[block], qu_laid[...])
        turns = table[rows, :]
        for head in range(heads):
            at = head * head_width
            q_heads[head, rows, :NOPE] = full[:, at : at + NOPE].astype(jnp.bfloat16)
            part = full[:, at + NOPE : at + head_width]
            q_heads[head, rows, NOPE:] = turned(part, turns).astype(jnp.bfloat16)
        return 0

    lax.fori_loop(0, sp_count, make_block, 0)
    wo.relay()

    factor = (NOPE + ROPE) ** (-0.5) * math.log2(math.e)
    contract = (((1,), (1,)), ((), ()))
    width = heads * VDIM

    def back(block):
        return pltpu.make_async_remote_copy(
            src_ref=attended.at[block],
            dst_ref=merged.at[:, pl.ds(pl.multiple_of(me * width, LANES), width)],
            send_sem=back_send.at[block],
            recv_sem=back_recv.at[me],
            device_id={"sp": block},
            device_id_type=MESH,
        )

    for block in reversed(range(sp_count)):
        begin = block * count

        def one_head(head, _):
            query = q_heads[head, begin : begin + count, :]
            near = lax.dot_general(
                query, k_heads[head, begin : begin + count, :], contract,
                preferred_element_type=jnp.float32,
            )
            row = lax.broadcasted_iota(jnp.int32, near.shape, 0)
            col = lax.broadcasted_iota(jnp.int32, near.shape, 1)
            near = jnp.where(col <= row, near, -jnp.inf)
            top = jnp.max(near, axis=-1, keepdims=True)
            if block:
                far = lax.dot_general(
                    query, k_heads[head, :begin, :], contract, preferred_element_type=jnp.float32
                )
                top = jnp.maximum(top, jnp.max(far, axis=-1, keepdims=True))
            near = jnp.exp2((near - top) * factor)
            total = jnp.sum(near, axis=-1, keepdims=True)
            if block:
                far = jnp.exp2((far - top) * factor)
                total = total + jnp.sum(far, axis=-1, keepdims=True)
            share = 1.0 / total
            result = dot((near * share).astype(jnp.bfloat16), v_heads[head, begin : begin + count, :])
            if block:
                result = result + dot((far * share).astype(jnp.bfloat16), v_heads[head, :begin, :])
            lanes = pl.ds(pl.multiple_of(head * VDIM, LANES), VDIM)
            attended[block, :, lanes] = result.astype(jnp.bfloat16)
            return 0

        lax.fori_loop(0, heads, one_head, 0)

        @pl.when(me != block)
        def _():
            back(block).start()

        @pl.when(me == block)
        def _():
            merged[:, pl.ds(pl.multiple_of(me * width, LANES), width)] = attended[block]

    wo.cross()
    wo.finish()
    for source in range(sp_count):

        @pl.when(me != source)
        def _():
            pltpu.make_async_remote_copy(
                src_ref=attended.at[source],
                dst_ref=merged.at[:, source * width : (source + 1) * width],
                send_sem=back_send.at[source],
                recv_sem=back_recv.at[source],
                device_id={"sp": source},
                device_id_type=MESH,
            ).wait()

    out_width = wo_all.shape[2]

    def project(piece, squares):
        value = dot(merged[...], wo_all[piece])
        proj[:, pl.ds(pl.multiple_of(piece * out_width, LANES), out_width)] = value
        return squares + jnp.sum(value * value, axis=-1, keepdims=True)

    squares = lax.fori_loop(0, dp_count, project, jnp.zeros((count, 1), jnp.float32))
    scale = lax.rsqrt(squares * (1.0 / proj.shape[1]) + EPSILON)
    out[...] = (proj[...] * scale * out_gain[...]).astype(jnp.bfloat16)
    for copy in copies.sent:
        copy.wait_send()


def kernel_body(mesh, tokens, w_qdown, w_kvdown, w_rotary, q_gain, kv_gain, w_qup, w_kvup, w_out, out_gain):
    sp_count, dp_count = mesh.shape["sp"], mesh.shape["dp"]
    heads = HEADS // sp_count
    count, depth = tokens.shape[1:]
    length = count * sp_count
    q_rank, kv_rank = w_qdown.shape[1], w_kvdown.shape[1]
    bf16 = jnp.bfloat16
    steps = dp_count // 2 - 1
    sems = 3 * (6 * steps + 1) + 2 * (2 * steps + 1) + 2 * 4
    sp_width = HEADS // sp_count
    result = pl.pallas_call(
        functools.partial(kernel, sp_count, dp_count),
        out_shape=jax.ShapeDtypeStruct((count, w_out.shape[1] * dp_count), bf16),
        in_specs=[pl.BlockSpec(memory_space=pltpu.VMEM)] * 11,
        out_specs=pl.BlockSpec(memory_space=pltpu.VMEM),
        scratch_shapes=[
            pltpu.VMEM((dp_count,) + w_qdown.shape, bf16),
            pltpu.VMEM((dp_count,) + w_kvdown.shape, bf16),
            pltpu.VMEM((dp_count, w_qup.shape[0], sp_width * (NOPE + ROPE)), bf16),
            pltpu.VMEM((dp_count, w_kvup.shape[0], sp_width * (NOPE + VDIM)), bf16),
            pltpu.VMEM((dp_count,) + w_out.shape, bf16),
            pltpu.VMEM((sp_count, count, q_rank), bf16),
            pltpu.VMEM((sp_count, count, kv_rank + 2 * ROPE), bf16),
            pltpu.VMEM((heads, length, NOPE + 2 * ROPE), bf16),
            pltpu.VMEM((heads, length, NOPE + 2 * ROPE), bf16),
            pltpu.VMEM((heads, length, VDIM), bf16),
            pltpu.VMEM((q_rank, heads * (NOPE + 2 * ROPE)), bf16),
            pltpu.VMEM((sp_count, count, heads * VDIM), bf16),
            pltpu.VMEM((count, HEADS * VDIM), bf16),
            pltpu.VMEM((count, w_out.shape[1] * dp_count), jnp.float32),
            pltpu.SemaphoreType.DMA((sems,)),
            pltpu.SemaphoreType.DMA((sems,)),
            pltpu.SemaphoreType.DMA((sp_count,)),
            pltpu.SemaphoreType.DMA((sp_count,)),
        ],
        compiler_params=pltpu.CompilerParams(
            collective_id=0, has_side_effects=True, vmem_limit_bytes=60 * 1024 * 1024
        ),
        name="latent_attention",
    )(
        tokens[0], w_qdown, w_kvdown, w_rotary, q_gain[None], kv_gain[None], w_qup, w_kvup, w_out,
        out_gain[None], jnp.asarray(turn_table(length)),
    )
    return result[None]


def fits_kernel(mesh):
    return mesh.shape["sp"] == 2 * 2 and mesh.shape["dp"] % 2 == 0


def solution(mesh):
    in_specs = (
        P("dp", "sp", None),
        P("dp", None),
        P("dp", None),
        P(),
        P(),
        P(),
        P("dp", None),
        P("dp", None),
        P(None, "dp"),
        P(),
    )
    out_specs = P("dp", "sp", None)
    body = functools.partial(kernel_body, mesh) if fits_kernel(mesh) else plain_body
    return jax.shard_map(body, mesh=mesh, in_specs=in_specs, out_specs=out_specs, check_vma=False)
```

```python
import functools
import math

import jax
import jax.numpy as jnp
import numpy as np
from jax import lax
from jax.experimental import pallas as pl
from jax.experimental.pallas import tpu as pltpu
from jax.sharding import PartitionSpec as P

HEADS = 16
NOPE = 128
ROPE = 64
VDIM = 128


EPSILON = 1e-06
THETA = 10000.0
LANES = 128
SUBLANES = 16
MESH = pl.DeviceIdType.MESH


def norm_rows(values, gain):
    scale = lax.rsqrt(jnp.mean(values * values, axis=-1, keepdims=True) + EPSILON)
    return values * scale * gain


def rotate(values, cosine, sine):
    half = values.shape[-1] // 2
    first = values[..., :half]
    second = values[..., half:]
    return jnp.concatenate(
        [first * cosine - second * sine, second * cosine + first * sine], axis=-1
    )


def turn_tables(offset, count):
    positions = (offset + jnp.arange(count)).astype(jnp.float32)
    freqs = THETA ** (-jnp.arange(0, ROPE, 2).astype(jnp.float32) / ROPE)
    angles = positions[:, None] * freqs[None, :]
    return (jnp.cos(angles), jnp.sin(angles))


def make_queries(q_full, cosine, sine, heads_here):
    rows = q_full.shape[0]
    shaped = q_full.reshape(rows, heads_here, NOPE + ROPE)
    turned = rotate(shaped[..., NOPE:], cosine[:, None, :], sine[:, None, :])
    joined = jnp.concatenate([shaped[..., :NOPE], turned], axis=-1)
    return joined.reshape(rows, heads_here * (NOPE + ROPE)).astype(jnp.bfloat16)


def attend(query_heads, keyval_heads, key_rot, heads_here):
    length = query_heads.shape[0]
    block = math.gcd(length, 512)
    scaling = (NOPE + ROPE) ** (-0.5)
    queries = query_heads.reshape(length, heads_here, NOPE + ROPE)
    keyval = keyval_heads.reshape(length, heads_here, NOPE + VDIM)
    keys_all = keyval[..., :NOPE]
    values_all = keyval[..., NOPE:]
    outputs = []
    for begin in range(0, length, block):
        finish = begin + block
        query_block = queries[begin:finish]
        scores = jnp.einsum(
            "qhd,khd->hqk",
            query_block[..., :NOPE],
            keys_all[:finish],
            preferred_element_type=jnp.float32,
        )
        scores = scores + jnp.einsum(
            "qhd,kd->hqk",
            query_block[..., NOPE:],
            key_rot[:finish],
            preferred_element_type=jnp.float32,
        )
        scores = scores * scaling
        query_pos = begin + jnp.arange(block)
        key_pos = jnp.arange(finish)
        allowed = key_pos[None, :] <= query_pos[:, None]
        scores = jnp.where(allowed[None], scores, -jnp.inf)
        top = jnp.max(scores, axis=-1, keepdims=True)
        expo = jnp.exp(scores - top)
        weights = (expo / jnp.sum(expo, axis=-1, keepdims=True)).astype(jnp.bfloat16)
        attended = jnp.einsum(
            "hqk,khd->qhd", weights, values_all[:finish], preferred_element_type=jnp.float32
        )
        outputs.append(attended.astype(jnp.bfloat16))
    return jnp.concatenate(outputs, axis=0).reshape(length, heads_here * VDIM)


def plain_body(tokens, w_qdown, w_kvdown, w_rotary, q_gain, kv_gain, w_qup, w_kvup, w_out, out_gain):
    own_rows = tokens[0]
    tok_count = own_rows.shape[0]
    sp_count = lax.axis_size("sp")
    sp_place = lax.axis_index("sp")
    length = tok_count * sp_count
    heads_here = HEADS // sp_count
    pieces = (
        lax.all_gather(w_qdown, "dp", axis=0, tiled=True),
        lax.all_gather(w_kvdown, "dp", axis=0, tiled=True),
    )
    q_lat = jnp.dot(own_rows, pieces[0], preferred_element_type=jnp.float32)
    kv_lat = jnp.dot(own_rows, pieces[1], preferred_element_type=jnp.float32)
    q_norm = norm_rows(q_lat, q_gain).astype(jnp.bfloat16)
    kv_norm = norm_rows(kv_lat, kv_gain).astype(jnp.bfloat16)
    own_cos, own_sin = turn_tables(sp_place * tok_count, tok_count)
    key_rot = rotate(
        jnp.dot(own_rows, w_rotary, preferred_element_type=jnp.float32), own_cos, own_sin
    ).astype(jnp.bfloat16)
    q_all, kv_all, rot_all = (
        lax.all_gather(q_norm, "sp", axis=0, tiled=True),
        lax.all_gather(kv_norm, "sp", axis=0, tiled=True),
        lax.all_gather(key_rot, "sp", axis=0, tiled=True),
    )
    q_width = heads_here * (NOPE + ROPE)
    kv_width = heads_here * (NOPE + VDIM)
    q_columns = lax.dynamic_slice_in_dim(w_qup, sp_place * q_width, q_width, 1)
    kv_columns = lax.dynamic_slice_in_dim(w_kvup, sp_place * kv_width, kv_width, 1)
    pieces = (
        lax.all_gather(q_columns, "dp", axis=0, tiled=True),
        lax.all_gather(kv_columns, "dp", axis=0, tiled=True),
    )
    q_full = jnp.dot(q_all, pieces[0], preferred_element_type=jnp.float32)
    kv_full = jnp.dot(kv_all, pieces[1], preferred_element_type=jnp.float32)
    all_cos, all_sin = turn_tables(0, length)
    query_heads = make_queries(q_full, all_cos, all_sin, heads_here)
    keyval_heads = kv_full.astype(jnp.bfloat16)
    attended = attend(query_heads, keyval_heads, rot_all, heads_here)
    merged = lax.all_to_all(attended, "sp", split_axis=0, concat_axis=1, tiled=True)
    proj = jnp.dot(
        merged, lax.all_gather(w_out, "dp", axis=1, tiled=True), preferred_element_type=jnp.float32
    )
    mixed = norm_rows(proj, out_gain).astype(jnp.bfloat16)
    return mixed[None]


def turn_table(length):
    positions = np.arange(length, dtype=np.float32)
    freqs = np.float32(THETA) ** (-np.arange(0, ROPE, 2).astype(np.float32) / np.float32(ROPE))
    angles = positions[:, None] * freqs[None, :].astype(np.float32)
    cosine, sine = np.cos(angles), np.sin(angles)
    return np.concatenate([cosine, cosine, sine, sine], axis=1).astype(np.float32)


class Copies:
    def __init__(self, send_sems, recv_sems):
        self.send_sems, self.recv_sems = send_sems, recv_sems
        self.used = 0
        self.sent = []

    def start(self, source, target, device):
        at = self.used
        self.used += 1
        copy = pltpu.make_async_remote_copy(
            src_ref=source,
            dst_ref=target,
            send_sem=self.send_sems.at[at],
            recv_sem=self.recv_sems.at[at],
            device_id=device,
            device_id_type=MESH,
        )
        copy.start()
        self.sent.append(copy)
        return copy


class PlaneSpread:
    def __init__(self, copies, place, view, rows):
        self.copies, self.place, self.view, self.rows = copies, place, view, rows

    def send(self):
        me, rows = self.place["me"], self.rows
        block = self.view(me, 0, rows)
        self.along_x = self.copies.start(block, block, {"sp": self.place["x"]})
        self.along_y = self.copies.start(block, block, {"sp": self.place["y"]})

    def relay(self):
        half = self.rows // 2
        self.along_x.wait_recv()
        block = self.view(self.place["x"], 0, half)
        self.first = self.copies.start(block, block, {"sp": self.place["y"]})
        self.along_y.wait_recv()
        block = self.view(self.place["y"], half, half)
        self.second = self.copies.start(block, block, {"sp": self.place["x"]})

    def finish(self):
        self.first.wait_recv()
        self.second.wait_recv()


class WeightGather:
    def __init__(self, copies, place, source, buffer, local_sem):
        self.copies, self.place, self.source, self.buffer = copies, place, source, buffer
        self.rows = source.shape[0] // place["sp_count"]
        self.local_sem = local_sem
        self.steps = range(1, place["z_count"])
        self.planes = {}

    def piece(self, slot, owner, begin, count):
        start = pl.multiple_of(owner * self.rows + begin, SUBLANES)
        return self.buffer.at[slot, pl.ds(start, count), :]

    def start(self):
        place, rows = self.place, self.rows
        own = self.source.at[pl.ds(pl.multiple_of(place["me"] * rows, SUBLANES), rows), :]
        self.arrivals = {}
        for step in self.steps:
            target = self.piece(place["dp"], place["me"], 0, rows)
            device = {"dp": lax.rem(place["dp"] + 2 * step, place["dp_count"])}
            self.arrivals[step] = self.copies.start(own, target, device)

    def keep(self):
        place = self.place
        self.crossed = [
            self.copies.start(self.source, self.buffer.at[place["dp"]], {"dp": place["core"]})
        ]
        self.local = None
        if self.local_sem is None:
            self.buffer[place["dp"]] = self.source[...]
        else:
            self.local = pltpu.make_async_copy(
                self.source, self.buffer.at[place["dp"]], self.local_sem
            )
            self.local.start()

    def slot(self, step):
        place = self.place
        return lax.rem(place["dp"] + place["dp_count"] - 2 * step, place["dp_count"])

    def cross(self, step, owner):
        block = self.piece(self.slot(step), owner, 0, self.rows)
        self.crossed.append(self.copies.start(block, block, {"dp": self.place["core"]}))

    def spread(self, step):
        self.arrivals[step].wait_recv()
        view = functools.partial(self.piece, self.slot(step))
        plane = PlaneSpread(self.copies, self.place, view, self.rows)
        plane.send()
        self.planes[step] = plane
        self.cross(step, self.place["me"])

    def relay(self, step):
        self.planes[step].relay()
        self.cross(step, self.place["x"])
        self.cross(step, self.place["y"])

    def close(self, step):
        self.planes[step].finish()
        self.cross(step, self.place["far"])

    def finish(self):
        if self.local is not None:
            self.local.wait()
        for copy in self.crossed:
            copy.wait_recv()


class ColumnGather:
    def __init__(self, copies, place, source, buffer, local_sem):
        self.copies, self.place, self.source, self.buffer = copies, place, source, buffer
        self.local_sem = local_sem
        width = buffer.shape[2]
        self.columns = pl.ds(pl.multiple_of(place["me"] * width, LANES), width)

    def start(self):
        place = self.place
        own = self.source.at[:, self.columns]
        target = self.buffer.at[place["dp"]]
        self.arrivals = []
        for step in range(1, place["z_count"]):
            device = {"dp": lax.rem(place["dp"] + 2 * step, place["dp_count"])}
            self.arrivals.append(self.copies.start(own, target, device))

    def keep(self):
        place = self.place
        own = self.source.at[:, self.columns]
        target = self.buffer.at[place["dp"]]
        self.crossed = [self.copies.start(own, target, {"dp": place["core"]})]
        self.local = pltpu.make_async_copy(own, target, self.local_sem)
        self.local.start()

    def cross(self):
        place = self.place
        for step in range(1, place["z_count"]):
            self.arrivals[step - 1].wait_recv()
            slot = lax.rem(place["dp"] + place["dp_count"] - 2 * step, place["dp_count"])
            block = self.buffer.at[slot]
            self.crossed.append(self.copies.start(block, block, {"dp": place["core"]}))

    def finish(self):
        self.local.wait()
        for copy in self.crossed:
            copy.wait_recv()


def rotary_picks(rows, offset, skip):
    width = skip + 2 * ROPE
    row = lax.broadcasted_iota(jnp.int32, (rows, width), 0)
    col = lax.broadcasted_iota(jnp.int32, (rows, width), 1)
    half = ROPE // 2
    minus = (col >= skip + ROPE) & (col < skip + ROPE + half)
    origin = jnp.where(
        col < skip + ROPE, col, jnp.where(minus, col - half, col - ROPE - half)
    )
    sign = jnp.where(minus, -1.0, 1.0)
    return jnp.where(row == origin + offset, sign, 0.0).astype(jnp.bfloat16)


def turned(values, table):
    product = values * table
    return product + pltpu.roll(product, ROPE, axis=1)


def dot(left, right):
    return jnp.dot(left, right, preferred_element_type=jnp.float32)


def kernel(
    sp_count, dp_count,
    tokens, w_qdown, w_kvdown, w_rotary, q_gain, kv_gain, w_qup, w_kvup, w_out, out_gain, table,
    out,
    qd_all, kvd_all, qu_all, kvu_all, wo_all, q_lat, kv_lat,
    q_heads, k_heads, v_heads, qu_laid, attended, merged,
    send_sems, recv_sems, back_send, back_recv, local_sems,
):
    me = lax.axis_index("sp")
    dp = lax.axis_index("dp")
    place = {
        "me": me,
        "dp": dp,
        "sp_count": sp_count,
        "dp_count": dp_count,
        "z_count": dp_count // 2,
        "x": me + 1 - 2 * lax.rem(me, 2),
        "y": lax.rem(me + 2, sp_count),
        "far": sp_count - 1 - me,
        "core": dp + 1 - 2 * lax.rem(dp, 2),
    }
    count = tokens.shape[0]
    heads = q_heads.shape[0]
    rank = kvd_all.shape[2]

    barrier = pltpu.get_barrier_semaphore()
    peers = [{"sp": lax.rem(me + step, sp_count)} for step in range(1, sp_count)]
    peers += [{"dp": lax.rem(dp + 2 * step, dp_count)} for step in range(1, dp_count // 2)]
    peers += [{"dp": place["core"]}]
    for peer in peers:
        pl.semaphore_signal(barrier, inc=1, device_id=peer, device_id_type=MESH)
    pl.semaphore_wait(barrier, len(peers))

    copies = Copies(send_sems, recv_sems)
    kvd = WeightGather(copies, place, w_kvdown, kvd_all, None)
    qd = WeightGather(copies, place, w_qdown, qd_all, None)
    kvu = ColumnGather(copies, place, w_kvup, kvu_all, local_sems.at[0])
    qu = ColumnGather(copies, place, w_qup, qu_all, local_sems.at[1])
    wo = WeightGather(copies, place, w_out, wo_all, local_sems.at[2])
    gathers = (kvd, qd, kvu, qu, wo)
    for gather in gathers:
        gather.start()
    for gather in gathers:
        gather.keep()

    own_table = table[pl.ds(pl.multiple_of(me * count, SUBLANES), count), :]
    picks = rotary_picks(ROPE, 0, 0)
    rotary = lax.dot_general(
        picks, w_rotary[...], (((0,), (0,)), ((), ())), preferred_element_type=jnp.float32
    ).astype(jnp.bfloat16)
    key_rot = lax.dot_general(
        tokens[...], rotary, (((1,), (1,)), ((), ())), preferred_element_type=jnp.float32
    )
    key_rot = turned(key_rot, own_table)
    lane = lax.broadcasted_iota(jnp.int32, key_rot.shape, 1)
    key_rot = jnp.where(lane < ROPE, key_rot, 0.0).astype(jnp.bfloat16)
    kv_lat[me, :, rank:] = key_rot

    steps = kvd.steps
    for step in steps:
        kvd.spread(step)
    for step in steps:
        kvd.relay(step)
        qd.spread(step)
    for step in steps:
        kvd.close(step)
        qd.relay(step)
    kvd.finish()
    down = kvd_all[...].reshape(-1, rank)
    kv_lat[me, :, :rank] = norm_rows(dot(tokens[...], down), kv_gain[...]).astype(jnp.bfloat16)

    def block_view(buffer, owner, begin, rows):
        return buffer.at[owner, pl.ds(begin, rows), :]

    kv_plane = PlaneSpread(copies, place, functools.partial(block_view, kv_lat), count)
    q_plane = PlaneSpread(copies, place, functools.partial(block_view, q_lat), count)
    kv_plane.send()
    for step in steps:
        qd.close(step)
    qd.finish()
    down = qd_all[...].reshape(-1, qd_all.shape[2])
    q_lat[me] = norm_rows(dot(tokens[...], down), q_gain[...]).astype(jnp.bfloat16)
    q_plane.send()
    kv_plane.relay()

    qu.cross()
    kvu.cross()
    qu.finish()
    laid = qu_all[...].reshape(-1, qu_all.shape[2])
    head_width = NOPE + 2 * ROPE
    for head in range(heads):
        picks = rotary_picks(laid.shape[1], head * (NOPE + ROPE), NOPE)
        qu_laid[:, head * head_width : (head + 1) * head_width] = dot(laid, picks).astype(
            jnp.bfloat16
        )
    q_plane.relay()
    kvu.finish()
    kv_plane.finish()

    def make_keys(block, _):
        rows = pl.ds(pl.multiple_of(block * count, SUBLANES), count)
        latent = kv_lat[block]
        full = dot(latent[:, :rank], kvu_all[...].reshape(rank, -1)).astype(jnp.bfloat16)
        for head in range(heads):
            at = head * (NOPE + VDIM)
            k_heads[head, rows, :NOPE] = full[:, at : at + NOPE]
            k_heads[head, rows, NOPE:] = latent[:, rank:]
            v_heads[head, rows, :] = full[:, at + NOPE : at + NOPE + VDIM]
        return 0

    lax.fori_loop(0, sp_count, make_keys, 0)
    q_plane.finish()
    wo.spread(1)

    def make_block(block, _):
        rows = pl.ds(pl.multiple_of(block * count, SUBLANES), count)
        full = dot(q_lat[block], qu_laid[...])
        turns = table[rows, :]
        for head in range(heads):
            at = head * head_width
            q_heads[head, rows, :NOPE] = full[:, at : at + NOPE].astype(jnp.bfloat16)
            part = full[:, at + NOPE : at + head_width]
            q_heads[head, rows, NOPE:] = turned(part, turns).astype(jnp.bfloat16)
        return 0

    lax.fori_loop(0, sp_count, make_block, 0)

    chores = [functools.partial(wo.spread, step) for step in steps if step > 1]
    chores += [functools.partial(wo.relay, step) for step in steps]
    chores_now = -(-len(chores) // sp_count)

    factor = (NOPE + ROPE) ** (-0.5) * math.log2(math.e)
    contract = (((1,), (1,)), ((), ()))
    width = heads * VDIM

    def back(block):
        return pltpu.make_async_remote_copy(
            src_ref=attended.at[block],
            dst_ref=merged.at[:, pl.ds(pl.multiple_of(me * width, LANES), width)],
            send_sem=back_send.at[block],
            recv_sem=back_recv.at[me],
            device_id={"sp": block},
            device_id_type=MESH,
        )

    for block in reversed(range(sp_count)):
        begin = block * count

        def one_head(head, _):
            query = q_heads[head, begin : begin + count, :]
            near = lax.dot_general(
                query, k_heads[head, begin : begin + count, :], contract,
                preferred_element_type=jnp.float32,
            )
            row = lax.broadcasted_iota(jnp.int32, near.shape, 0)
            col = lax.broadcasted_iota(jnp.int32, near.shape, 1)
            near = jnp.where(col <= row, near, -jnp.inf)
            top = jnp.max(near, axis=-1, keepdims=True)
            if block:
                far = lax.dot_general(
                    query, k_heads[head, :begin, :], contract, preferred_element_type=jnp.float32
                )
                top = jnp.maximum(top, jnp.max(far, axis=-1, keepdims=True))
            near = jnp.exp2((near - top) * factor)
            total = jnp.sum(near, axis=-1, keepdims=True)
            if block:
                far = jnp.exp2((far - top) * factor)
                total = total + jnp.sum(far, axis=-1, keepdims=True)
            share = 1.0 / total
            result = dot((near * share).astype(jnp.bfloat16), v_heads[head, begin : begin + count, :])
            if block:
                result = result + dot((far * share).astype(jnp.bfloat16), v_heads[head, :begin, :])
            lanes = pl.ds(pl.multiple_of(head * VDIM, LANES), VDIM)
            attended[block, :, lanes] = result.astype(jnp.bfloat16)
            return 0

        lax.fori_loop(0, heads, one_head, 0)

        @pl.when(me != block)
        def _():
            back(block).start()

        @pl.when(me == block)
        def _():
            merged[:, pl.ds(pl.multiple_of(me * width, LANES), width)] = attended[block]

        for chore in chores[:chores_now]:
            chore()
        del chores[:chores_now]

    for step in steps:
        wo.close(step)
    wo.finish()
    for source in range(sp_count):

        @pl.when(me != source)
        def _():
            pltpu.make_async_remote_copy(
                src_ref=attended.at[source],
                dst_ref=merged.at[:, source * width : (source + 1) * width],
                send_sem=back_send.at[source],
                recv_sem=back_recv.at[source],
                device_id={"sp": source},
                device_id_type=MESH,
            ).wait()

    out_width = wo_all.shape[2]

    def project(piece, squares):
        lanes = pl.ds(pl.multiple_of(piece * out_width, LANES), out_width)
        value = dot(merged[...], wo_all[piece])
        out[:, lanes] = value
        return squares + jnp.sum(value * value, axis=-1, keepdims=True)

    squares = lax.fori_loop(0, dp_count, project, jnp.zeros((count, 1), jnp.float32))
    scale = lax.rsqrt(squares * (1.0 / out.shape[1]) + EPSILON)
    out[...] = out[...] * scale * out_gain[...]
    for copy in copies.sent:
        copy.wait_send()


def kernel_body(mesh, tokens, w_qdown, w_kvdown, w_rotary, q_gain, kv_gain, w_qup, w_kvup, w_out, out_gain):
    sp_count, dp_count = mesh.shape["sp"], mesh.shape["dp"]
    heads = HEADS // sp_count
    count, depth = tokens.shape[1:]
    length = count * sp_count
    q_rank, kv_rank = w_qdown.shape[1], w_kvdown.shape[1]
    bf16 = jnp.bfloat16
    steps = dp_count // 2 - 1
    sems = 3 * (9 * steps + 1) + 2 * (2 * steps + 1) + 2 * 4
    vmem, hbm = pl.BlockSpec(memory_space=pltpu.VMEM), pl.BlockSpec(memory_space=pl.ANY)
    sp_width = HEADS // sp_count
    mixed = pl.pallas_call(
        functools.partial(kernel, sp_count, dp_count),
        out_shape=jax.ShapeDtypeStruct((count, w_out.shape[1] * dp_count), jnp.float32),
        in_specs=[vmem] * 6 + [hbm] * 3 + [vmem] * 2,
        out_specs=vmem,
        scratch_shapes=[
            pltpu.VMEM((dp_count,) + w_qdown.shape, bf16),
            pltpu.VMEM((dp_count,) + w_kvdown.shape, bf16),
            pltpu.VMEM((dp_count, w_qup.shape[0], sp_width * (NOPE + ROPE)), bf16),
            pltpu.VMEM((dp_count, w_kvup.shape[0], sp_width * (NOPE + VDIM)), bf16),
            pltpu.VMEM((dp_count,) + w_out.shape, bf16),
            pltpu.VMEM((sp_count, count, q_rank), bf16),
            pltpu.VMEM((sp_count, count, kv_rank + 2 * ROPE), bf16),
            pltpu.VMEM((heads, length, NOPE + 2 * ROPE), bf16),
            pltpu.VMEM((heads, length, NOPE + 2 * ROPE), bf16),
            pltpu.VMEM((heads, length, VDIM), bf16),
            pltpu.VMEM((q_rank, heads * (NOPE + 2 * ROPE)), bf16),
            pltpu.VMEM((sp_count, count, heads * VDIM), bf16),
            pltpu.VMEM((count, HEADS * VDIM), bf16),
            pltpu.SemaphoreType.DMA((sems,)),
            pltpu.SemaphoreType.DMA((sems,)),
            pltpu.SemaphoreType.DMA((sp_count,)),
            pltpu.SemaphoreType.DMA((sp_count,)),
            pltpu.SemaphoreType.DMA((3,)),
        ],
        compiler_params=pltpu.CompilerParams(
            collective_id=0, has_side_effects=True, vmem_limit_bytes=60 * 1024 * 1024
        ),
        name="latent_attention",
    )(
        tokens[0], w_qdown, w_kvdown, w_rotary.T, q_gain[None], kv_gain[None], w_qup, w_kvup, w_out,
        out_gain[None], jnp.asarray(turn_table(length)),
    )
    return mixed.astype(bf16)[None]


def fits_kernel(mesh):
    return mesh.shape["sp"] == 2 * 2 and mesh.shape["dp"] % 2 == 0


def solution(mesh):
    in_specs = (
        P("dp", "sp", None),
        P("dp", None),
        P("dp", None),
        P(),
        P(),
        P(),
        P("dp", None),
        P("dp", None),
        P(None, "dp"),
        P(),
    )
    out_specs = P("dp", "sp", None)
    body = functools.partial(kernel_body, mesh) if fits_kernel(mesh) else plain_body
    return jax.shard_map(body, mesh=mesh, in_specs=in_specs, out_specs=out_specs, check_vma=False)
```
